32 devices in a mesh: sp: 8 (over z, x), tp: 4 (over y, core).
Axes of the slice: x: 2, y: 2, z: 4, core: 2. Of those that a mesh axis runs over, the one named last changes fastest.
Arguments:
- resid: bfloat16 [2048, 4096], P(('sp', 'tp')), may hold values from -6 to 6
- queries: bfloat16 [2048, 2048], P('sp', 'tp'), may hold values from -6 to 6
- keys: bfloat16 [2048, 512], P('sp', 'tp'), may hold values from -6 to 6
- values: bfloat16 [2048, 512], P('sp', 'tp'), may hold values from -6 to 6
- q_gain: float32 [128], replicated, may hold values from 0.5 to 6
- key_norm_gain: float32 [128], replicated, may hold values from 0.5 to 6
- out_weight: bfloat16 [2048, 4096], P('tp'), may hold values from -0.125 to 0.125
- norm1_gain: float32 [4096], replicated, may hold values from 0.1 to 1.9
- norm2_gain: float32 [4096], replicated, may hold values from 0.1 to 1.9
- expert_ids: int32 [2048, 2], P(('sp', 'tp')), may hold values from 0 to 7, all different within a row; in each aligned block of 64 rows (0 to 63, 64 to 127, ...) at most 24 rows name the same one
- group_weight: float32 [2048], P(('sp', 'tp')), may hold values from 0.3 to 1
- expert_weight: float32 [2048, 2], P(('sp', 'tp')), may hold values from 0.1 to 1
- gate_proj: bfloat16 [8, 4096, 1024], P('sp', None, 'tp'), may hold values from -0.09375 to 0.09375
- up_proj: bfloat16 [8, 4096, 1024], P('sp', None, 'tp'), may hold values from -0.09375 to 0.09375
- down_proj: bfloat16 [8, 1024, 4096], P('sp', 'tp'), may hold values from -0.1875 to 0.1875
Outputs:
- mixed_out: bfloat16 [2048, 4096], P(('sp', 'tp'))
The draws below stay inside these ranges and needn't reach their ends.
Inputs may be any that keep to these rules, and one draw needn't show every extreme that they name: `expert_ids`: each row names 2 different experts. Among the rows of one device (aligned blocks of 64 rows) no expert is named by more than 24 rows, a bound that some block reaches.
All inputs are finite; a program needn't handle non-finite values.
Results may differ from the reference program's by a relative error of at most 0.012.
The reference program's roundings to bfloat16 on the way count: a program that leaves them out, or rounds other values in their place, can miss the bound.
Values may be sent and summed in bfloat16 or wider, within the bound.
A program may use at most 192 MiB of HBM per device.

```python
import math
import jax
import jax.numpy as jnp
import numpy as np
from jax import lax

D = 4096
HEAD_WIDTH = 128
QUERY_HEADS = 16
KEY_VALUE_HEADS = 4
GRID_W = 64
FF = 1024
TOP = 2
SEQUENCE_TOKENS = 2048
ROWS_DEV = 64
EXPERTS = 8
CAP = 24
N_SP = 8
N_TP = 4


def gain_law(key):
    return jax.random.uniform(key, (HEAD_WIDTH,), jnp.float32, 0.5, 2.0)


def draw_q_gain(key, part):
    return gain_law(jax.random.fold_in(key, 31))


def draw_key_norm_gain(key, part):
    return gain_law(jax.random.fold_in(key, 37))


def key_table(key):
    sampled_values = jax.random.normal(jax.random.fold_in(key, 41), (SEQUENCE_TOKENS, KEY_VALUE_HEADS * HEAD_WIDTH), jnp.float32)
    return jnp.clip(sampled_values, -6.0, 6.0)


def draw_keys(key, part):
    return key_table(key).astype(jnp.bfloat16)


def draw_queries(key, part):
    sampled_values = jax.random.normal(jax.random.fold_in(key, 43), (SEQUENCE_TOKENS, QUERY_HEADS * HEAD_WIDTH), jnp.float32)
    sampled_values = jnp.clip(sampled_values, -6.0, 6.0)
    return sampled_values.astype(jnp.bfloat16)


def block_scale(stream_key, shape, split, low, high):
    def one(dim, parts):
        draws = jax.random.uniform(jax.random.fold_in(jax.random.fold_in(stream_key, 6), dim), (parts,), jnp.float32, low / len(split), high / len(split))
        return jnp.repeat(jnp.exp(draws), shape[dim] // parts).reshape((-1,) + (1,) * (len(shape) - dim - 1))

    loudness = one(*split[0])
    for cut in split[1:]:
        loudness = loudness * one(*cut)
    return loudness


def routed_block(own_key, own, number, rows, amount, top, reach, lean):
    ranking = jax.random.permutation(own_key, amount)
    heavy_load, common = load_shares(amount, rows * top, reach, lean, True), load_shares(amount, rows * top, reach, lean, False)
    places = jnp.arange(amount)

    def named(tallies, turn):
        used = int((tallies > 0).sum())
        fixed = max(1, used // 4)
        shifted = fixed + (places - fixed + turn * (used - fixed)) % max(1, amount - fixed)
        return jnp.zeros((amount,), jnp.int32).at[ranking[jnp.where(places < fixed, places, shifted)]].set(jnp.asarray(tallies, jnp.int32))

    tallies = jnp.where(number % 4 == 0, named(heavy_load, number // 4), named(common, number - number // 4 - 1))
    mixed = jax.random.permutation(jax.random.fold_in(own, 3), amount)
    donor, sink = mixed[0:amount // 2 * 2:2], mixed[1:amount // 2 * 2:2]
    slack = jnp.minimum(tallies[donor] - 1, reach - tallies[sink]) // 2
    slack = jnp.where((donor == ranking[0]) | (sink == ranking[0]) | (tallies[sink] == 0), 0, jnp.maximum(slack, 0))
    shifted = jax.random.randint(jax.random.fold_in(own, 4), (amount // 2,), 0, 1 << 20) % (slack + 1)
    tallies = tallies.at[donor].add(-shifted).at[sink].add(shifted)
    items = jnp.searchsorted(jnp.cumsum(tallies), jnp.arange(rows * top), side="right").astype(jnp.int32)
    table = items.reshape(top, rows).T
    table = table[jax.random.permutation(jax.random.fold_in(own, 1), rows)]
    turn = jax.random.randint(jax.random.fold_in(own, 2), (rows, 1), 0, top)
    return jnp.take_along_axis(table, (jnp.arange(top)[None, :] + turn) % top, axis=1)


def load_shares(count, total, bound, skew, full):
    weights = [(1 << 20) // math.isqrt(grade ** skew) + 1 for grade in range(1, count + 1)]
    largest = bound if full else min(bound, max(-(-total // count), total * weights[0] // sum(weights)))
    least = 1 if total - largest >= count - 1 else 0
    holding, surplus = [largest] + [least] * (count - 1), total - largest - least * (count - 1)
    while surplus > 0:
        free = [i for i in range(1, count) if holding[i] < largest] or [i for i in range(1, count) if holding[i] < bound]
        whole, left = sum([weights[i] for i in free]), surplus
        for i in free:
            more = min(bound - holding[i], max(1, left * weights[i] // whole), surplus)
            holding[i] = holding[i] + more
            surplus = surplus - more
    return np.array(holding)


def normal_values(rng, dims, deviation, bound, split=(), kind=jnp.bfloat16):
    values = deviation * jax.random.normal(rng, dims, jnp.float32)
    if split:
        values = values * block_scale(rng, dims, split, -0.22, 0.18)
    return jnp.clip(values, -bound, bound).astype(kind)


def setup_inputs(seed: int = 0) -> dict:
    streams_of = jax.random.split(jax.random.key(seed), 16)
    resid = normal_values(streams_of[0], (SEQUENCE_TOKENS, D), 1.0, 6.0, ((0, 32),))
    queries = draw_queries(jax.random.fold_in(streams_of[15], 71), 0)
    keys = draw_keys(jax.random.fold_in(streams_of[15], 71), 0)
    values = normal_values(streams_of[3], (SEQUENCE_TOKENS, KEY_VALUE_HEADS * HEAD_WIDTH), 1.0, 6.0, ((0, 8), (1, 4)))
    q_gain = draw_q_gain(jax.random.fold_in(streams_of[15], 71), 0)
    key_norm_gain = draw_key_norm_gain(jax.random.fold_in(streams_of[15], 71), 0)
    out_weight = normal_values(streams_of[6], (QUERY_HEADS * HEAD_WIDTH, D), (QUERY_HEADS * HEAD_WIDTH) ** -0.5, 0.125, ((0, 4),))
    norm1_gain = jnp.clip(1.0 + 0.18 * jax.random.normal(streams_of[7], (D,), jnp.float32), 0.1, 1.9)
    norm2_gain = jnp.clip(1.0 + 0.18 * jax.random.normal(streams_of[8], (D,), jnp.float32), 0.1, 1.9)
    expert_ids_keys = jax.random.split(jax.random.fold_in(streams_of[9], 1), SEQUENCE_TOKENS // ROWS_DEV)
    expert_ids_turns = jax.random.permutation(jax.random.fold_in(streams_of[9], 3), SEQUENCE_TOKENS // ROWS_DEV)
    expert_ids = jax.vmap(lambda own, number: routed_block(jax.random.fold_in(streams_of[9], 2), own, number, ROWS_DEV, EXPERTS, TOP, CAP, 1))(expert_ids_keys, expert_ids_turns).reshape((SEQUENCE_TOKENS, TOP))
    group_weight = jnp.clip(0.3 + 0.7 * jax.random.uniform(streams_of[10], (SEQUENCE_TOKENS,), jnp.float32) ** block_scale(streams_of[10], (SEQUENCE_TOKENS,), ((0, 32),), -0.2, 0.2), 0.3, 1.0)
    expert_weight = jnp.clip(0.1 + 0.9 * jax.random.uniform(streams_of[11], (SEQUENCE_TOKENS, TOP), jnp.float32) ** block_scale(streams_of[11], (SEQUENCE_TOKENS, TOP), ((0, 32),), -0.2, 0.2), 0.1, 1.0)
    gate_proj = normal_values(streams_of[12], (EXPERTS, D, FF), D ** -0.5, 0.09375, ((0, 8), (2, 4)))
    up_proj = normal_values(streams_of[13], (EXPERTS, D, FF), D ** -0.5, 0.09375, ((0, 8), (2, 4)))
    down_proj = normal_values(streams_of[14], (EXPERTS, FF, D), FF ** -0.5, 0.1875, ((0, 8), (1, 4)))
    return dict(resid=resid, queries=queries, keys=keys, values=values, q_gain=q_gain, key_norm_gain=key_norm_gain, out_weight=out_weight, norm1_gain=norm1_gain, norm2_gain=norm2_gain, expert_ids=expert_ids, group_weight=group_weight, expert_weight=expert_weight, gate_proj=gate_proj, up_proj=up_proj, down_proj=down_proj)


deep_alpha = 2.0 ** 0.5
rope_theta = 10000.0

def apply_rotary_heads(block, gain, grid_positions):
    values32 = block.astype(jnp.float32)
    normed = values32 * lax.rsqrt(lax.optimization_barrier(jnp.mean(values32 * values32, -1, keepdims=True)) + 1e-06) * gain
    half = normed.shape[-1] // 2
    inv_freq = rope_theta ** (-jnp.arange(0, half, 2, dtype=jnp.float32) / half)
    grid_row = (grid_positions // GRID_W).astype(jnp.float32)
    grid_col = (grid_positions % GRID_W).astype(jnp.float32)
    angle = jnp.concatenate([grid_row[:, None] * inv_freq, grid_col[:, None] * inv_freq], -1)[:, None, :]
    cosine = jnp.cos(angle)
    sine = jnp.sin(angle)
    first = normed[..., :half]
    second = normed[..., half:]
    turned = jnp.concatenate([first * cosine - second * sine, first * sine + second * cosine], -1)
    return turned.astype(jnp.bfloat16)

def layer_norm_gain(summed, gain):
    centre = summed - lax.optimization_barrier(jnp.mean(summed, -1, keepdims=True))
    spread = lax.optimization_barrier(jnp.mean(centre * centre, -1, keepdims=True))
    return centre * lax.rsqrt(spread + 1e-06) * gain

def reference(resid, queries, keys, values, q_gain, key_norm_gain, out_weight, norm1_gain, norm2_gain, expert_ids, group_weight, expert_weight, gate_proj, up_proj, down_proj):
    grid_positions = jnp.arange(SEQUENCE_TOKENS, dtype=jnp.int32)
    query_group = QUERY_HEADS // KEY_VALUE_HEADS
    q_rot = apply_rotary_heads(queries.reshape(SEQUENCE_TOKENS, QUERY_HEADS, HEAD_WIDTH), q_gain, grid_positions)
    rotated_keys = apply_rotary_heads(keys.reshape(SEQUENCE_TOKENS, KEY_VALUE_HEADS, HEAD_WIDTH), key_norm_gain, grid_positions).astype(jnp.float32)
    value_rows_full = values.reshape(SEQUENCE_TOKENS, KEY_VALUE_HEADS, HEAD_WIDTH).astype(jnp.float32)
    query_extent = math.gcd(SEQUENCE_TOKENS, 128)

    def attend(query_tile):
        query_widened = query_tile.reshape(query_extent, KEY_VALUE_HEADS, query_group, HEAD_WIDTH).astype(jnp.float32)
        scores = jnp.einsum('qkgd,lkd->kgql', query_widened, rotated_keys) * HEAD_WIDTH ** (-0.5)
        row_max = lax.optimization_barrier(jnp.max(scores, -1, keepdims=True))
        weights = jnp.exp(scores - row_max)
        row_sum = lax.optimization_barrier(jnp.sum(weights, -1))
        rounded = lax.optimization_barrier(weights.astype(jnp.bfloat16)).astype(jnp.float32)
        mixed = jnp.einsum('kgql,lkd->qkgd', rounded, value_rows_full)
        mixed = mixed / jnp.transpose(row_sum, (2, 0, 1))[..., None]
        return mixed.reshape(query_extent, QUERY_HEADS * HEAD_WIDTH).astype(jnp.bfloat16)
    attn = lax.map(attend, q_rot.reshape(SEQUENCE_TOKENS // query_extent, query_extent, QUERY_HEADS, HEAD_WIDTH)).reshape(SEQUENCE_TOKENS, QUERY_HEADS * HEAD_WIDTH)
    proj = jnp.dot(attn, out_weight, preferred_element_type=jnp.float32).astype(jnp.bfloat16)
    summed = deep_alpha * resid.astype(jnp.float32) + proj.astype(jnp.float32)
    x_one = layer_norm_gain(summed, norm1_gain).astype(jnp.bfloat16)
    gates = group_weight[:, None] * expert_weight / lax.optimization_barrier(jnp.sum(expert_weight, -1, keepdims=True))
    copies = SEQUENCE_TOKENS * TOP
    most_rows = CAP * N_SP * N_TP
    ff_dev = FF // N_TP
    flat_ids = expert_ids.reshape(-1)
    gate_flat = jnp.concatenate([gates.reshape(-1), jnp.zeros((1,), jnp.float32)])
    x_padded = jnp.concatenate([x_one, jnp.zeros((1, D), jnp.bfloat16)], 0)

    def per_expert(total, expert):
        index = jnp.nonzero(flat_ids == expert, size=most_rows, fill_value=copies)[0].astype(jnp.int32)
        token_index = jnp.where(index < copies, index // TOP, SEQUENCE_TOKENS).astype(jnp.int32)
        chosen = x_padded[token_index]
        w_gate = lax.dynamic_index_in_dim(gate_proj, expert, 0, keepdims=False)
        w_up = lax.dynamic_index_in_dim(up_proj, expert, 0, keepdims=False)
        w_down = lax.dynamic_index_in_dim(down_proj, expert, 0, keepdims=False)
        gate_part = jnp.dot(chosen, w_gate, preferred_element_type=jnp.float32)
        up_part = jnp.dot(chosen, w_up, preferred_element_type=jnp.float32)
        hidden = (jax.nn.silu(gate_part) * up_part).astype(jnp.bfloat16)
        expert_sum = jnp.zeros((most_rows, D), jnp.float32)
        for lane in range(N_TP):
            partial_sum = jnp.dot(hidden[:, lane * ff_dev:(lane + 1) * ff_dev], w_down[lane * ff_dev:(lane + 1) * ff_dev], preferred_element_type=jnp.float32)
            rounded = lax.optimization_barrier(partial_sum.astype(jnp.bfloat16))
            expert_sum = expert_sum + rounded.astype(jnp.float32)
        expert_out = expert_sum.astype(jnp.bfloat16).astype(jnp.float32)
        weighted = gate_flat[index][:, None] * expert_out
        return (total.at[token_index].add(weighted), None)
    start_total = jnp.zeros((SEQUENCE_TOKENS + 1, D), jnp.float32)
    moe_total, _ = lax.scan(per_expert, start_total, jnp.arange(EXPERTS, dtype=jnp.int32))
    moe = moe_total[:SEQUENCE_TOKENS]
    final = deep_alpha * x_one.astype(jnp.float32) + moe
    return layer_norm_gain(final, norm2_gain).astype(jnp.bfloat16)
```

```python
import functools

import jax
import jax.numpy as jnp
from jax import lax
from jax.experimental import pallas as pl
from jax.experimental.pallas import tpu as pltpu
from jax.sharding import PartitionSpec as P

GRID_W = 64


deep_alpha = 2.0**0.5
rope_theta = 10000.0


def apply_rotary_heads(block, gain, grid_positions):
    values32 = block.astype(jnp.float32)
    normed = values32 * lax.rsqrt(jnp.mean(values32 * values32, -1, keepdims=True) + 1e-06) * gain
    half = normed.shape[-1] // 2
    inv_freq = rope_theta ** (-jnp.arange(0, half, 2, dtype=jnp.float32) / half)
    grid_row = (grid_positions // GRID_W).astype(jnp.float32)
    grid_col = (grid_positions % GRID_W).astype(jnp.float32)
    angle = jnp.concatenate([grid_row[:, None] * inv_freq, grid_col[:, None] * inv_freq], -1)[
        :, None, :
    ]
    cosine = jnp.cos(angle)
    sine = jnp.sin(angle)
    first = normed[..., :half]
    second = normed[..., half:]
    turned = jnp.concatenate([first * cosine - second * sine, first * sine + second * cosine], -1)
    return turned.astype(jnp.bfloat16)


def layer_norm_gain(summed, gain):
    centre = summed - jnp.mean(summed, -1, keepdims=True)
    spread = jnp.mean(centre * centre, -1, keepdims=True)
    return centre * lax.rsqrt(spread + 1e-06) * gain


MESH = pl.DeviceIdType.MESH


def flip_bits(a, b, size):
    out = 0
    bit = 1
    while bit < size:
        out = out + ((a // bit + b // bit) % 2) * bit
        bit *= 2
    return out


def at_sp(index):
    return {"sp": index}


def at_tp(index):
    return {"tp": index}


def tp_partners(n_tp):
    t = lax.axis_index("tp")
    t1 = t + 1 - 2 * (t % 2)
    t2 = (t + n_tp // 2) % n_tp
    t3 = (t1 + n_tp // 2) % n_tp
    return t, t1, t2, t3


def attn_kernel(n_sp, heads, kv_heads, width, exponent_scale, q_ref, kv_ref, o_ref, slots, m_s, l_s, acc, send, recv):
    me = lax.axis_index("sp")
    pair = me + 1 - 2 * (me % 2)
    group = heads // kv_heads

    barrier = pltpu.get_barrier_semaphore()
    pl.semaphore_signal(barrier, inc=1, device_id=at_sp(pair), device_id_type=MESH)

    def greet(j, _):
        pl.semaphore_signal(
            barrier, inc=1, device_id=at_sp(flip_bits(me, 2 * j, n_sp)), device_id_type=MESH
        )
        return 0

    lax.fori_loop(1, n_sp // 2, greet, 0)
    pl.semaphore_wait(barrier, n_sp // 2)

    def copy(src, slot, target):
        return pltpu.make_async_remote_copy(
            src_ref=src,
            dst_ref=slots.at[slot],
            send_sem=send.at[slot],
            recv_sem=recv.at[slot],
            device_id=at_sp(target),
            device_id_type=MESH,
        )

    copy(kv_ref, 1, pair).start()

    def spread(j, _):
        copy(kv_ref, 2 * j, flip_bits(me, 2 * j, n_sp)).start()
        return 0

    lax.fori_loop(1, n_sp // 2, spread, 0)

    m_s[...] = jnp.full(m_s.shape, -1e30, jnp.float32)
    l_s[...] = jnp.zeros(l_s.shape, jnp.float32)
    acc[...] = jnp.zeros(acc.shape, jnp.float32)

    def process(block):
        for h in range(heads):
            g = h // group
            q = q_ref[:, h * width : (h + 1) * width]
            k = block[:, g * width : (g + 1) * width]
            v = block[:, (kv_heads + g) * width : (kv_heads + g + 1) * width]
            s = lax.dot_general(q, k, (((1,), (1,)), ((), ())), preferred_element_type=jnp.float32)
            m_prev = m_s[h]
            m_new = jnp.maximum(m_prev, jnp.max(s, -1, keepdims=True))
            m_s[h] = m_new
            alpha = jnp.exp2((m_prev - m_new) * exponent_scale)
            p = jnp.exp2((s - m_new[:, :1]) * exponent_scale)
            l_s[h] = l_s[h] * alpha + jnp.sum(p, -1, keepdims=True)
            acc[h] = acc[h] * alpha + jnp.dot(
                p.astype(jnp.bfloat16), v, preferred_element_type=jnp.float32
            )

    process(kv_ref)

    def step(j, _):
        even = 2 * j + 2
        copy(kv_ref, even, pair).wait_recv()
        copy(slots.at[even], even + 1, pair).start()
        copy(kv_ref, even - 1, pair).wait_recv()
        process(slots.at[even - 1])
        process(slots.at[even])
        return 0

    lax.fori_loop(0, n_sp // 2 - 1, step, 0)
    copy(kv_ref, n_sp - 1, pair).wait_recv()
    process(slots.at[n_sp - 1])
    for h in range(heads):
        o_ref[:, h * width : (h + 1) * width] = (acc[h] / l_s[h]).astype(jnp.bfloat16)

    def drain(slot, _):
        copy(kv_ref, slot, pair).wait_send()
        return 0

    lax.fori_loop(1, n_sp, drain, 0)


def attend(q_rot, kv, n_sp, heads, kv_heads, width):
    rows = q_rot.shape[0]
    return pl.pallas_call(
        functools.partial(
            attn_kernel, n_sp, heads, kv_heads, width, width ** (-0.5) * 1.4426950408889634
        ),
        out_shape=jax.ShapeDtypeStruct((rows, heads * width), jnp.bfloat16),
        in_specs=[pl.BlockSpec(memory_space=pltpu.VMEM)] * 2,
        out_specs=pl.BlockSpec(memory_space=pltpu.VMEM),
        scratch_shapes=[
            pltpu.VMEM((n_sp,) + kv.shape, jnp.bfloat16),
            pltpu.VMEM((heads, rows, 128), jnp.float32),
            pltpu.VMEM((heads, rows, 128), jnp.float32),
            pltpu.VMEM((heads, rows, width), jnp.float32),
            pltpu.SemaphoreType.DMA((n_sp,)),
            pltpu.SemaphoreType.DMA((n_sp,)),
        ],
        compiler_params=pltpu.CompilerParams(collective_id=0, has_side_effects=True),
        name="attend",
    )(q_rot, kv)


def dispatch_kernel(n_sp, n_tp, out_ref, piece, stage, local, send, recv):
    me = lax.axis_index("sp")
    t, t1, t2, t3 = tp_partners(n_tp)

    barrier = pltpu.get_barrier_semaphore()
    pl.semaphore_signal(barrier, inc=1, device_id=at_tp(t1), device_id_type=MESH)
    pl.semaphore_signal(barrier, inc=1, device_id=at_tp(t2), device_id_type=MESH)

    def greet(k, _):
        pl.semaphore_signal(
            barrier, inc=1, device_id=at_sp(flip_bits(me, k, n_sp)), device_id_type=MESH
        )
        return 0

    lax.fori_loop(1, n_sp, greet, 0)
    pl.semaphore_wait(barrier, n_sp + 1)

    def copy(src, owner, source, kind, k, target):
        return pltpu.make_async_remote_copy(
            src_ref=src,
            dst_ref=piece.at[source, owner],
            send_sem=send.at[kind, k],
            recv_sem=recv.at[kind, k],
            device_id=target,
            device_id_type=MESH,
        )

    mine = out_ref.at[me]
    keep = pltpu.make_async_copy(mine, stage, local.at[0])
    keep.start()
    copy(mine, t, me, 2, 0, at_tp(t2)).start()
    copy(mine, t, me, 1, 0, at_tp(t1)).start()

    def spread(k, _):
        other = flip_bits(me, k, n_sp)
        copy(out_ref.at[other], t, me, 0, k, at_sp(other)).start()
        return 0

    lax.fori_loop(1, n_sp, spread, 0)
    keep.wait()
    put = pltpu.make_async_copy(stage, piece.at[me, t], local.at[1])
    put.start()

    def relay(k):
        source = flip_bits(me, k, n_sp)
        copy(mine, t2, source, 2, k, at_tp(t2)).wait_recv()
        copy(piece.at[source, t2], t2, source, 3, k, at_tp(t1)).start()

    def forward(k, _):
        source = flip_bits(me, k, n_sp)
        copy(mine, t, source, 0, k, at_tp(t1)).wait_recv()
        copy(piece.at[source, t], t, source, 2, k, at_tp(t2)).start()
        copy(piece.at[source, t], t, source, 1, k, at_tp(t1)).start()
        relay(k - 1)
        return 0

    lax.fori_loop(1, n_sp, forward, 0)
    relay(n_sp - 1)

    def drain(k, _):
        source = flip_bits(me, k, n_sp)
        copy(mine, t1, source, 1, k, at_tp(t1)).wait()
        copy(mine, t2, source, 2, k, at_tp(t2)).wait_send()
        copy(mine, t3, source, 3, k, at_tp(t1)).wait()
        return 0

    lax.fori_loop(0, n_sp, drain, 0)

    def drain_first(k, _):
        copy(mine, t, me, 0, k, at_tp(t1)).wait_send()
        return 0

    lax.fori_loop(1, n_sp, drain_first, 0)
    put.wait()


def dispatch(outgoing, n_sp, n_tp):
    block = outgoing.shape[1:]
    return pl.pallas_call(
        functools.partial(dispatch_kernel, n_sp, n_tp),
        out_shape=jax.ShapeDtypeStruct((n_sp, n_tp) + block, jnp.bfloat16),
        in_specs=[pl.BlockSpec(memory_space=pl.ANY)],
        out_specs=pl.BlockSpec(memory_space=pl.ANY),
        scratch_shapes=[
            pltpu.VMEM(block, jnp.bfloat16),
            pltpu.SemaphoreType.DMA((2,)),
            pltpu.SemaphoreType.DMA((4, n_sp)),
            pltpu.SemaphoreType.DMA((4, n_sp)),
        ],
        compiler_params=pltpu.CompilerParams(collective_id=1, has_side_effects=True),
        name="dispatch",
    )(outgoing)


def reduce_kernel(steps, n_tp, back, part, out, from_core, from_pair, pair_sum, total, send, recv):
    me = lax.axis_index("sp")
    t, t1, t2, t3 = tp_partners(n_tp)

    barrier = pltpu.get_barrier_semaphore()
    pl.semaphore_signal(barrier, inc=1, device_id=at_tp(t1), device_id_type=MESH)
    pl.semaphore_signal(barrier, inc=1, device_id=at_tp(t2), device_id_type=MESH)
    if back:

        def greet(k, _):
            pl.semaphore_signal(
                barrier, inc=1, device_id=at_sp(flip_bits(me, k, steps)), device_id_type=MESH
            )
            return 0

        lax.fori_loop(1, steps, greet, 0)
        pl.semaphore_wait(barrier, steps + 1)
    else:
        pl.semaphore_wait(barrier, 2)

    def order(i):
        return steps - 1 - i

    def block_of(k, lane):
        return flip_bits(me, k, steps) * n_tp + lane if back else lane * steps + k

    def copy(src, dst, kind, k, target):
        return pltpu.make_async_remote_copy(
            src_ref=src,
            dst_ref=dst,
            send_sem=send.at[kind, k],
            recv_sem=recv.at[kind, k],
            device_id=target,
            device_id_type=MESH,
        )

    def core_copy(k, half):
        lane = t3 if half else t1
        return copy(part.at[block_of(k, lane)], from_core.at[k, half], half, k, at_tp(t1))

    def pair_copy(k):
        return copy(pair_sum.at[k], from_pair.at[k], 2, k, at_tp(t2))

    def back_copy(k):
        return copy(total.at[k], out.at[me], 3, k, at_sp(flip_bits(me, k, steps)))

    def first(i, _):
        k = order(i)
        core_copy(k, 1).start()
        core_copy(k, 0).start()
        return 0

    lax.fori_loop(0, steps, first, 0)

    width = part.shape[-1]
    strip = 512 if width % 512 == 0 else width

    def add_pair(k):
        core_copy(k, 1).wait_recv()
        own = block_of(k, t2)
        for c in range(0, width, strip):
            cols = slice(c, c + strip)
            pair_sum[k, :, cols] = (
                part[own, :, cols].astype(jnp.float32)
                + from_core[k, 1, :, cols].astype(jnp.float32)
            ).astype(jnp.bfloat16)
        pair_copy(k).start()

    def add_all(k, dst, row):
        core_copy(k, 0).wait_recv()
        pair_copy(k).wait_recv()
        own = block_of(k, t)
        for c in range(0, width, strip):
            cols = slice(c, c + strip)
            dst[row, :, cols] = (
                part[own, :, cols].astype(jnp.float32)
                + from_core[k, 0, :, cols].astype(jnp.float32)
                + from_pair[k, :, cols].astype(jnp.float32)
            ).astype(jnp.bfloat16)

    def finish(k):
        if back:
            add_all(k, total, k)
            back_copy(k).start()
        else:
            add_all(k, out, k)

    depth = min(2, steps - 1)
    for i in range(depth):
        add_pair(order(i))

    def middle(i, _):
        add_pair(order(i))
        finish(order(i - depth))
        return 0

    lax.fori_loop(depth, steps, middle, 0)
    for i in range(steps - depth, steps - 1):
        finish(order(i))
    if back:
        add_all(0, out, me)
    else:
        finish(0)

    def drain(k, _):
        core_copy(k, 0).wait_send()
        core_copy(k, 1).wait_send()
        pair_copy(k).wait_send()
        return 0

    lax.fori_loop(0, steps, drain, 0)
    if back:

        def drain_back(k, _):
            back_copy(k).wait()
            return 0

        lax.fori_loop(1, steps, drain_back, 0)


def reduce_lanes(part, steps, n_tp, back, collective_id):
    block = part.shape[1:]
    slots = pltpu.VMEM((steps,) + block, jnp.bfloat16)
    return pl.pallas_call(
        functools.partial(reduce_kernel, steps, n_tp, back),
        out_shape=jax.ShapeDtypeStruct((steps,) + block, jnp.bfloat16),
        in_specs=[pl.BlockSpec(memory_space=pltpu.VMEM)],
        out_specs=pl.BlockSpec(memory_space=pltpu.VMEM),
        scratch_shapes=[
            pltpu.VMEM((steps, 2) + block, jnp.bfloat16),
            slots,
            slots,
            slots if back else pltpu.VMEM((1,) + block, jnp.bfloat16),
            pltpu.SemaphoreType.DMA((4, steps)),
            pltpu.SemaphoreType.DMA((4, steps)),
        ],
        compiler_params=pltpu.CompilerParams(collective_id=collective_id, has_side_effects=True),
        name="reduce_back" if back else "reduce_proj",
    )(part)


def per_device(
    resid,
    queries,
    keys,
    values,
    q_gain,
    key_norm_gain,
    out_weight,
    norm1_gain,
    norm2_gain,
    expert_ids,
    group_weight,
    expert_weight,
    gate_proj,
    up_proj,
    down_proj,
):
    local_tokens = queries.shape[0]
    head_size = q_gain.shape[0]
    kv_local = keys.shape[1] // head_size
    query_group = queries.shape[1] // head_size // kv_local
    model_width = resid.shape[1]
    grid_positions = lax.axis_index("sp") * local_tokens + jnp.arange(local_tokens, dtype=jnp.int32)
    q_rot = apply_rotary_heads(
        queries.reshape(local_tokens, kv_local * query_group, head_size), q_gain, grid_positions
    )
    q_rot = q_rot.reshape(local_tokens, kv_local * query_group * head_size)
    rotated_keys = apply_rotary_heads(
        keys.reshape(local_tokens, kv_local, head_size), key_norm_gain, grid_positions
    )
    rotated_keys = rotated_keys.reshape(local_tokens, kv_local * head_size)
    lanes = lax.axis_size("tp")
    sp_count = lax.axis_size("sp")
    own_rows = local_tokens // lanes
    kv = jnp.concatenate([rotated_keys, values], 1)
    attn = attend(q_rot, kv, sp_count, kv_local * query_group, kv_local, head_size)
    proj_part = jnp.dot(attn, out_weight, preferred_element_type=jnp.float32).astype(jnp.bfloat16)
    proj_rows = 16
    proj_steps = own_rows // proj_rows
    proj = reduce_lanes(
        proj_part.reshape(lanes * proj_steps, proj_rows, model_width), proj_steps, lanes, False, 2
    )
    proj = proj.reshape(own_rows, model_width)
    summed = deep_alpha * resid.astype(jnp.float32) + proj.astype(jnp.float32)
    x_one = layer_norm_gain(summed, norm1_gain).astype(jnp.bfloat16)
    top_count = expert_ids.shape[1]
    expert_local = gate_proj.shape[0]
    expert_total = expert_local * sp_count
    capacity = (3 * top_count * own_rows + 2 * expert_total - 1) // (2 * expert_total)
    flat_ids = expert_ids.reshape(-1)
    one_hot = (flat_ids[:, None] == jnp.arange(expert_total, dtype=jnp.int32)[None, :]).astype(
        jnp.int32
    )
    earlier = jnp.cumsum(one_hot, 0) - one_hot
    rank = jnp.sum(earlier * one_hot, 1)
    slot = flat_ids * capacity + rank
    placing = slot[:, None] == jnp.arange(expert_total * capacity, dtype=jnp.int32)[None, :]
    placing = placing.astype(jnp.bfloat16).reshape(own_rows, top_count, expert_total * capacity)
    placing = jnp.sum(placing, 1)
    outgoing = lax.dot_general(
        placing, x_one, (((0,), (0,)), ((), ())), preferred_element_type=jnp.float32
    ).astype(jnp.bfloat16)
    outgoing = outgoing.reshape(expert_total, capacity, model_width)
    blocks = outgoing.reshape(sp_count, expert_local * capacity, model_width)
    piece = dispatch(blocks, sp_count, lanes)
    piece = piece.reshape(sp_count * lanes, expert_local, capacity, model_width)
    gate_part = jnp.einsum("recd,edf->recf", piece, gate_proj, preferred_element_type=jnp.float32)
    up_part = jnp.einsum("recd,edf->recf", piece, up_proj, preferred_element_type=jnp.float32)
    hidden = (jax.nn.silu(gate_part) * up_part).astype(jnp.bfloat16)
    partial_sum = jnp.einsum("recf,efd->recd", hidden, down_proj, preferred_element_type=jnp.float32)
    rounded = partial_sum.astype(jnp.bfloat16)
    rounded = rounded.reshape(sp_count * lanes, expert_local * capacity, model_width)
    returned = reduce_lanes(rounded, sp_count, lanes, True, 3)
    returned = returned.reshape(expert_total * capacity, model_width)
    picked_out = returned[slot].reshape(own_rows, top_count, model_width)
    gates = group_weight[:, None] * expert_weight / jnp.sum(expert_weight, -1, keepdims=True)
    moe = jnp.sum(gates[..., None] * picked_out.astype(jnp.float32), 1)
    final = deep_alpha * x_one.astype(jnp.float32) + moe
    return layer_norm_gain(final, norm2_gain).astype(jnp.bfloat16)


def solution(mesh):
    in_specs = (
        P(("sp", "tp"), None),
        P("sp", "tp"),
        P("sp", "tp"),
        P("sp", "tp"),
        P(),
        P(),
        P("tp", None),
        P(),
        P(),
        P(("sp", "tp"), None),
        P(("sp", "tp")),
        P(("sp", "tp"), None),
        P("sp", None, "tp"),
        P("sp", None, "tp"),
        P("sp", "tp", None),
    )
    out_specs = P(("sp", "tp"), None)
    return jax.shard_map(
        per_device, mesh=mesh, in_specs=in_specs, out_specs=out_specs, check_vma=False
    )
```

```python
import functools

import jax
import jax.numpy as jnp
from jax import lax
from jax.experimental import pallas as pl
from jax.experimental.pallas import tpu as pltpu
from jax.sharding import PartitionSpec as P

GRID_W = 64


deep_alpha = 2.0**0.5
rope_theta = 10000.0


def apply_rotary_heads(block, gain, grid_positions):
    values32 = block.astype(jnp.float32)
    normed = values32 * lax.rsqrt(jnp.mean(values32 * values32, -1, keepdims=True) + 1e-06) * gain
    half = normed.shape[-1] // 2
    inv_freq = rope_theta ** (-jnp.arange(0, half, 2, dtype=jnp.float32) / half)
    grid_row = (grid_positions // GRID_W).astype(jnp.float32)
    grid_col = (grid_positions % GRID_W).astype(jnp.float32)
    angle = jnp.concatenate([grid_row[:, None] * inv_freq, grid_col[:, None] * inv_freq], -1)[
        :, None, :
    ]
    cosine = jnp.cos(angle)
    sine = jnp.sin(angle)
    first = normed[..., :half]
    second = normed[..., half:]
    turned = jnp.concatenate([first * cosine - second * sine, first * sine + second * cosine], -1)
    return turned.astype(jnp.bfloat16)


def layer_norm_gain(summed, gain):
    centre = summed - jnp.mean(summed, -1, keepdims=True)
    spread = jnp.mean(centre * centre, -1, keepdims=True)
    return centre * lax.rsqrt(spread + 1e-06) * gain


MESH = pl.DeviceIdType.MESH


def flip_bits(a, b, size):
    out = 0
    bit = 1
    while bit < size:
        out = out + ((a // bit + b // bit) % 2) * bit
        bit *= 2
    return out


def at_sp(index):
    return {"sp": index}


def at_tp(index):
    return {"tp": index}


def tp_partners(n_tp):
    t = lax.axis_index("tp")
    t1 = t + 1 - 2 * (t % 2)
    t2 = (t + n_tp // 2) % n_tp
    t3 = (t1 + n_tp // 2) % n_tp
    return t, t1, t2, t3


def attn_kernel(n_sp, heads, kv_heads, width, exponent_scale, q_ref, kv_ref, o_ref, slots, m_s, l_s, acc, send, recv):
    me = lax.axis_index("sp")
    pair = me + 1 - 2 * (me % 2)
    group = heads // kv_heads

    barrier = pltpu.get_barrier_semaphore()
    pl.semaphore_signal(barrier, inc=1, device_id=at_sp(pair), device_id_type=MESH)

    def greet(j, _):
        pl.semaphore_signal(
            barrier, inc=1, device_id=at_sp(flip_bits(me, 2 * j, n_sp)), device_id_type=MESH
        )
        return 0

    lax.fori_loop(1, n_sp // 2, greet, 0)
    pl.semaphore_wait(barrier, n_sp // 2)

    def copy(src, slot, target):
        return pltpu.make_async_remote_copy(
            src_ref=src,
            dst_ref=slots.at[slot],
            send_sem=send.at[slot],
            recv_sem=recv.at[slot],
            device_id=at_sp(target),
            device_id_type=MESH,
        )

    copy(kv_ref, 1, pair).start()

    def spread(j, _):
        copy(kv_ref, 2 * j, flip_bits(me, 2 * j, n_sp)).start()
        return 0

    lax.fori_loop(1, n_sp // 2, spread, 0)

    m_s[...] = jnp.full(m_s.shape, -1e30, jnp.float32)
    l_s[...] = jnp.zeros(l_s.shape, jnp.float32)
    acc[...] = jnp.zeros(acc.shape, jnp.float32)

    def process(block):
        for h in range(heads):
            g = h // group
            q = q_ref[:, h * width : (h + 1) * width]
            k = block[:, g * width : (g + 1) * width]
            v = block[:, (kv_heads + g) * width : (kv_heads + g + 1) * width]
            s = lax.dot_general(q, k, (((1,), (1,)), ((), ())), preferred_element_type=jnp.float32)
            m_prev = m_s[h]
            m_new = jnp.maximum(m_prev, jnp.max(s, -1, keepdims=True))
            m_s[h] = m_new
            alpha = jnp.exp2((m_prev - m_new) * exponent_scale)
            p = jnp.exp2((s - m_new[:, :1]) * exponent_scale)
            l_s[h] = l_s[h] * alpha + jnp.sum(p, -1, keepdims=True)
            acc[h] = acc[h] * alpha + jnp.dot(
                p.astype(jnp.bfloat16), v, preferred_element_type=jnp.float32
            )

    process(kv_ref)

    def step(j, _):
        even = 2 * j + 2
        copy(kv_ref, even, pair).wait_recv()
        copy(slots.at[even], even + 1, pair).start()
        copy(kv_ref, even - 1, pair).wait_recv()
        process(slots.at[even - 1])
        process(slots.at[even])
        return 0

    lax.fori_loop(0, n_sp // 2 - 1, step, 0)
    copy(kv_ref, n_sp - 1, pair).wait_recv()
    process(slots.at[n_sp - 1])
    for h in range(heads):
        o_ref[:, h * width : (h + 1) * width] = (acc[h] / l_s[h]).astype(jnp.bfloat16)

    def drain(slot, _):
        copy(kv_ref, slot, pair).wait_send()
        return 0

    lax.fori_loop(1, n_sp, drain, 0)


def attend(q_rot, kv, n_sp, heads, kv_heads, width):
    rows = q_rot.shape[0]
    return pl.pallas_call(
        functools.partial(
            attn_kernel, n_sp, heads, kv_heads, width, width ** (-0.5) * 1.4426950408889634
        ),
        out_shape=jax.ShapeDtypeStruct((rows, heads * width), jnp.bfloat16),
        in_specs=[pl.BlockSpec(memory_space=pltpu.VMEM)] * 2,
        out_specs=pl.BlockSpec(memory_space=pltpu.VMEM),
        scratch_shapes=[
            pltpu.VMEM((n_sp,) + kv.shape, jnp.bfloat16),
            pltpu.VMEM((heads, rows, 128), jnp.float32),
            pltpu.VMEM((heads, rows, 128), jnp.float32),
            pltpu.VMEM((heads, rows, width), jnp.float32),
            pltpu.SemaphoreType.DMA((n_sp,)),
            pltpu.SemaphoreType.DMA((n_sp,)),
        ],
        compiler_params=pltpu.CompilerParams(collective_id=0, has_side_effects=True),
        name="attend",
    )(q_rot, kv)


def moe_kernel(
    n_sp,
    n_tp,
    stride,
    out_ref,
    gate_hbm,
    up_hbm,
    down_hbm,
    back,
    w_gate,
    w_up,
    w_down,
    piece,
    rows,
    part,
    from_core,
    from_pair,
    pair_sum,
    total,
    local,
    send,
    recv,
):
    me = lax.axis_index("sp")
    t, t1, t2, t3 = tp_partners(n_tp)
    cap, width = out_ref.shape[1:]
    strip = 1024 if width % 1024 == 0 else width

    loads = [
        pltpu.make_async_copy(src, dst, local.at[i])
        for i, (src, dst) in enumerate(
            ((gate_hbm, w_gate), (up_hbm, w_up), (down_hbm, w_down), (out_ref.at[me], piece.at[me, t]))
        )
    ]
    for load in loads:
        load.start()

    barrier = pltpu.get_barrier_semaphore()
    pl.semaphore_signal(barrier, inc=1, device_id=at_tp(t1), device_id_type=MESH)
    pl.semaphore_signal(barrier, inc=1, device_id=at_tp(t2), device_id_type=MESH)

    def greet(k, _):
        pl.semaphore_signal(
            barrier, inc=1, device_id=at_sp(flip_bits(me, k, n_sp)), device_id_type=MESH
        )
        return 0

    lax.fori_loop(1, n_sp, greet, 0)
    pl.semaphore_wait(barrier, n_sp + 1)

    def order(i):
        return jnp.where(i < 2, i, 2 + (i - 2 + n_sp // 2 - 2) % max(n_sp - 2, 1))

    def copy(src, dst, kind, k, target):
        return pltpu.make_async_remote_copy(
            src_ref=src,
            dst_ref=dst,
            send_sem=send.at[kind, k],
            recv_sem=recv.at[kind, k],
            device_id=target,
            device_id_type=MESH,
        )

    def owner(k):
        return flip_bits(me, k, n_sp)

    def first_copy(k):
        return copy(out_ref.at[owner(k)], piece.at[me, t], 0, k, at_sp(owner(k)))

    def core_forward(k):
        return copy(piece.at[owner(k), t], piece.at[owner(k), t], 1, k, at_tp(t1))

    def pair_forward(k):
        return copy(piece.at[owner(k), t], piece.at[owner(k), t], 2, k, at_tp(t2))

    def relay_copy(k):
        return copy(piece.at[owner(k), t2], piece.at[owner(k), t2], 3, k, at_tp(t1))

    def core_part(k, half):
        lane = t3 if half else t1
        return copy(part.at[k, lane], from_core.at[k, half], 4 + half, k, at_tp(t1))

    def pair_part(k):
        return copy(pair_sum.at[k], from_pair.at[k], 6, k, at_tp(t2))

    def back_copy(k):
        return copy(total.at[k], back.at[me], 7, k, at_sp(owner(k)))

    copy(out_ref.at[me], piece.at[me, t], 2, 0, at_tp(t2)).start()
    copy(out_ref.at[me], piece.at[me, t], 1, 0, at_tp(t1)).start()

    def spread(i, _):
        first_copy(order(i)).start()
        return 0

    lax.fori_loop(1, n_sp, spread, 0)
    rows[...] = jnp.zeros(rows.shape, jnp.float32)
    for load in loads:
        load.wait()

    def stage_forward(k):
        first_copy(k).wait_recv()
        pair_forward(k).start()
        core_forward(k).start()

    def stage_relay(k):
        pair_forward(k).wait_recv()
        relay_copy(k).start()

    def stage_expert(k):
        core_forward(k).wait_recv()
        relay_copy(k).wait_recv()
        source = owner(k)
        for lane in range(n_tp):
            rows[lane * stride : lane * stride + cap, :] = piece[source, lane].astype(jnp.float32)
        gate = jnp.zeros((n_tp * stride, w_gate.shape[1]), jnp.float32)
        up = jnp.zeros((n_tp * stride, w_up.shape[1]), jnp.float32)
        for c in range(0, width, strip):
            x = rows[:, c : c + strip].astype(jnp.bfloat16)
            gate += jnp.dot(x, w_gate[c : c + strip, :], preferred_element_type=jnp.float32)
            up += jnp.dot(x, w_up[c : c + strip, :], preferred_element_type=jnp.float32)
        hidden = (gate / (1.0 + jnp.exp(-gate)) * up).astype(jnp.bfloat16)
        for c in range(0, width, strip):
            y = jnp.dot(hidden, w_down[:, c : c + strip], preferred_element_type=jnp.float32)
            for lane in range(n_tp):
                part[k, lane, :, c : c + strip] = y[lane * stride : lane * stride + cap].astype(
                    jnp.bfloat16
                )
        core_part(k, 1).start()
        core_part(k, 0).start()

    def stage_pair(k):
        core_part(k, 1).wait_recv()
        for c in range(0, width, strip):
            cols = slice(c, c + strip)
            pair_sum[k, :, cols] = (
                part[k, t2, :, cols].astype(jnp.float32)
                + from_core[k, 1, :, cols].astype(jnp.float32)
            ).astype(jnp.bfloat16)
        pair_part(k).start()

    def stage_total(k):
        core_part(k, 0).wait_recv()
        pair_part(k).wait_recv()

        def add(dst, row):
            for c in range(0, width, strip):
                cols = slice(c, c + strip)
                dst[row, :, cols] = (
                    part[k, t, :, cols].astype(jnp.float32)
                    + from_core[k, 0, :, cols].astype(jnp.float32)
                    + from_pair[k, :, cols].astype(jnp.float32)
                ).astype(jnp.bfloat16)

        @pl.when(k == 0)
        def _():
            add(back, me)

        @pl.when(k > 0)
        def _():
            add(total, k)
            back_copy(k).start()

    def tick(i, _):
        @pl.when(jnp.logical_and(i >= 1, i < n_sp))
        def _():
            stage_forward(order(i))

        @pl.when(jnp.logical_and(i >= 1, i < n_sp + 1))
        def _():
            stage_relay(order(i - 1))

        @pl.when(jnp.logical_and(i >= 2, i < n_sp + 2))
        def _():
            stage_expert(order(i - 2))

        @pl.when(jnp.logical_and(i >= 3, i < n_sp + 3))
        def _():
            stage_pair(order(i - 3))

        @pl.when(i >= 4)
        def _():
            stage_total(order(i - 4))

        return 0

    lax.fori_loop(0, n_sp + 4, tick, 0)

    def drain(k, _):
        core_forward(k).wait_send()
        pair_forward(k).wait_send()
        relay_copy(k).wait_send()
        core_part(k, 0).wait_send()
        core_part(k, 1).wait_send()
        pair_part(k).wait_send()
        return 0

    lax.fori_loop(0, n_sp, drain, 0)

    def drain_far(k, _):
        first_copy(k).wait_send()
        back_copy(k).wait()
        return 0

    lax.fori_loop(1, n_sp, drain_far, 0)


def experts(outgoing, gate_proj, up_proj, down_proj, n_sp, n_tp):
    block = outgoing.shape[1:]
    stride = (block[0] + 7) // 8 * 8
    slots = pltpu.VMEM((n_sp,) + block, jnp.bfloat16)
    lanes = pltpu.VMEM((n_sp, n_tp) + block, jnp.bfloat16)
    anywhere = pl.BlockSpec(memory_space=pl.ANY)
    return pl.pallas_call(
        functools.partial(moe_kernel, n_sp, n_tp, stride),
        out_shape=jax.ShapeDtypeStruct(outgoing.shape, jnp.bfloat16),
        in_specs=[pl.BlockSpec(memory_space=pltpu.VMEM), anywhere, anywhere, anywhere],
        out_specs=pl.BlockSpec(memory_space=pltpu.VMEM),
        scratch_shapes=[
            pltpu.VMEM(gate_proj.shape, jnp.bfloat16),
            pltpu.VMEM(up_proj.shape, jnp.bfloat16),
            pltpu.VMEM(down_proj.shape, jnp.bfloat16),
            lanes,
            pltpu.VMEM((n_tp * stride, block[1]), jnp.float32),
            lanes,
            pltpu.VMEM((n_sp, 2) + block, jnp.bfloat16),
            slots,
            slots,
            slots,
            pltpu.SemaphoreType.DMA((4,)),
            pltpu.SemaphoreType.DMA((8, n_sp)),
            pltpu.SemaphoreType.DMA((8, n_sp)),
        ],
        compiler_params=pltpu.CompilerParams(collective_id=1, has_side_effects=True),
        name="experts",
    )(outgoing, gate_proj, up_proj, down_proj)


def reduce_kernel(steps, n_tp, back, part, out, from_core, from_pair, pair_sum, total, send, recv):
    me = lax.axis_index("sp")
    t, t1, t2, t3 = tp_partners(n_tp)

    barrier = pltpu.get_barrier_semaphore()
    pl.semaphore_signal(barrier, inc=1, device_id=at_tp(t1), device_id_type=MESH)
    pl.semaphore_signal(barrier, inc=1, device_id=at_tp(t2), device_id_type=MESH)
    if back:

        def greet(k, _):
            pl.semaphore_signal(
                barrier, inc=1, device_id=at_sp(flip_bits(me, k, steps)), device_id_type=MESH
            )
            return 0

        lax.fori_loop(1, steps, greet, 0)
        pl.semaphore_wait(barrier, steps + 1)
    else:
        pl.semaphore_wait(barrier, 2)

    def order(i):
        return steps - 1 - i

    def block_of(k, lane):
        return flip_bits(me, k, steps) * n_tp + lane if back else lane * steps + k

    def copy(src, dst, kind, k, target):
        return pltpu.make_async_remote_copy(
            src_ref=src,
            dst_ref=dst,
            send_sem=send.at[kind, k],
            recv_sem=recv.at[kind, k],
            device_id=target,
            device_id_type=MESH,
        )

    def core_copy(k, half):
        lane = t3 if half else t1
        return copy(part.at[block_of(k, lane)], from_core.at[k, half], half, k, at_tp(t1))

    def pair_copy(k):
        return copy(pair_sum.at[k], from_pair.at[k], 2, k, at_tp(t2))

    def back_copy(k):
        return copy(total.at[k], out.at[me], 3, k, at_sp(flip_bits(me, k, steps)))

    def first(i, _):
        k = order(i)
        core_copy(k, 1).start()
        core_copy(k, 0).start()
        return 0

    lax.fori_loop(0, steps, first, 0)

    width = part.shape[-1]
    strip = 512 if width % 512 == 0 else width

    def add_pair(k):
        core_copy(k, 1).wait_recv()
        own = block_of(k, t2)
        for c in range(0, width, strip):
            cols = slice(c, c + strip)
            pair_sum[k, :, cols] = (
                part[own, :, cols].astype(jnp.float32)
                + from_core[k, 1, :, cols].astype(jnp.float32)
            ).astype(jnp.bfloat16)
        pair_copy(k).start()

    def add_all(k, dst, row):
        core_copy(k, 0).wait_recv()
        pair_copy(k).wait_recv()
        own = block_of(k, t)
        for c in range(0, width, strip):
            cols = slice(c, c + strip)
            dst[row, :, cols] = (
                part[own, :, cols].astype(jnp.float32)
                + from_core[k, 0, :, cols].astype(jnp.float32)
                + from_pair[k, :, cols].astype(jnp.float32)
            ).astype(jnp.bfloat16)

    def finish(k):
        if back:
            add_all(k, total, k)
            back_copy(k).start()
        else:
            add_all(k, out, k)

    depth = min(2, steps - 1)
    for i in range(depth):
        add_pair(order(i))

    def middle(i, _):
        add_pair(order(i))
        finish(order(i - depth))
        return 0

    lax.fori_loop(depth, steps, middle, 0)
    for i in range(steps - depth, steps - 1):
        finish(order(i))
    if back:
        add_all(0, out, me)
    else:
        finish(0)

    def drain(k, _):
        core_copy(k, 0).wait_send()
        core_copy(k, 1).wait_send()
        pair_copy(k).wait_send()
        return 0

    lax.fori_loop(0, steps, drain, 0)
    if back:

        def drain_back(k, _):
            back_copy(k).wait()
            return 0

        lax.fori_loop(1, steps, drain_back, 0)


def reduce_lanes(part, steps, n_tp, back, collective_id):
    block = part.shape[1:]
    slots = pltpu.VMEM((steps,) + block, jnp.bfloat16)
    return pl.pallas_call(
        functools.partial(reduce_kernel, steps, n_tp, back),
        out_shape=jax.ShapeDtypeStruct((steps,) + block, jnp.bfloat16),
        in_specs=[pl.BlockSpec(memory_space=pltpu.VMEM)],
        out_specs=pl.BlockSpec(memory_space=pltpu.VMEM),
        scratch_shapes=[
            pltpu.VMEM((steps, 2) + block, jnp.bfloat16),
            slots,
            slots,
            slots if back else pltpu.VMEM((1,) + block, jnp.bfloat16),
            pltpu.SemaphoreType.DMA((4, steps)),
            pltpu.SemaphoreType.DMA((4, steps)),
        ],
        compiler_params=pltpu.CompilerParams(collective_id=collective_id, has_side_effects=True),
        name="reduce_back" if back else "reduce_proj",
    )(part)


def per_device(
    resid,
    queries,
    keys,
    values,
    q_gain,
    key_norm_gain,
    out_weight,
    norm1_gain,
    norm2_gain,
    expert_ids,
    group_weight,
    expert_weight,
    gate_proj,
    up_proj,
    down_proj,
):
    local_tokens = queries.shape[0]
    head_size = q_gain.shape[0]
    kv_local = keys.shape[1] // head_size
    query_group = queries.shape[1] // head_size // kv_local
    model_width = resid.shape[1]
    grid_positions = lax.axis_index("sp") * local_tokens + jnp.arange(local_tokens, dtype=jnp.int32)
    q_rot = apply_rotary_heads(
        queries.reshape(local_tokens, kv_local * query_group, head_size), q_gain, grid_positions
    )
    q_rot = q_rot.reshape(local_tokens, kv_local * query_group * head_size)
    rotated_keys = apply_rotary_heads(
        keys.reshape(local_tokens, kv_local, head_size), key_norm_gain, grid_positions
    )
    rotated_keys = rotated_keys.reshape(local_tokens, kv_local * head_size)
    lanes = lax.axis_size("tp")
    sp_count = lax.axis_size("sp")
    own_rows = local_tokens // lanes
    kv = jnp.concatenate([rotated_keys, values], 1)
    attn = attend(q_rot, kv, sp_count, kv_local * query_group, kv_local, head_size)
    proj_part = jnp.dot(attn, out_weight, preferred_element_type=jnp.float32).astype(jnp.bfloat16)
    proj_rows = 16
    proj_steps = own_rows // proj_rows
    proj = reduce_lanes(
        proj_part.reshape(lanes * proj_steps, proj_rows, model_width), proj_steps, lanes, False, 2
    )
    proj = proj.reshape(own_rows, model_width)
    summed = deep_alpha * resid.astype(jnp.float32) + proj.astype(jnp.float32)
    x_one = layer_norm_gain(summed, norm1_gain).astype(jnp.bfloat16)
    top_count = expert_ids.shape[1]
    expert_local = gate_proj.shape[0]
    expert_total = expert_local * sp_count
    capacity = (3 * top_count * own_rows + 2 * expert_total - 1) // (2 * expert_total)
    flat_ids = expert_ids.reshape(-1)
    one_hot = (flat_ids[:, None] == jnp.arange(expert_total, dtype=jnp.int32)[None, :]).astype(
        jnp.int32
    )
    earlier = jnp.cumsum(one_hot, 0) - one_hot
    rank = jnp.sum(earlier * one_hot, 1)
    slot = flat_ids * capacity + rank
    chosen = slot[:, None] == jnp.arange(expert_total * capacity, dtype=jnp.int32)[None, :]
    chosen = chosen.reshape(own_rows, top_count, expert_total * capacity)
    placing = jnp.sum(chosen.astype(jnp.bfloat16), 1)
    outgoing = lax.dot_general(
        placing, x_one, (((0,), (0,)), ((), ())), preferred_element_type=jnp.float32
    ).astype(jnp.bfloat16)
    outgoing = outgoing.reshape(expert_total, capacity, model_width)
    blocks = outgoing.reshape(sp_count, expert_local * capacity, model_width)
    returned = experts(
        blocks,
        gate_proj.reshape(gate_proj.shape[1:]),
        up_proj.reshape(up_proj.shape[1:]),
        down_proj.reshape(down_proj.shape[1:]),
        sp_count,
        lanes,
    )
    returned = returned.reshape(expert_total * capacity, model_width)
    gates = group_weight[:, None] * expert_weight / jnp.sum(expert_weight, -1, keepdims=True)
    combine = jnp.sum(jnp.where(chosen, gates[..., None], 0.0), 1)
    high = lax.reduce_precision(combine, 8, 7)
    both = jnp.concatenate([high, combine - high], 0).astype(jnp.bfloat16)
    picked = jnp.dot(both, returned, preferred_element_type=jnp.float32)
    moe = picked[:own_rows] + picked[own_rows:]
    final = deep_alpha * x_one.astype(jnp.float32) + moe
    return layer_norm_gain(final, norm2_gain).astype(jnp.bfloat16)


def solution(mesh):
    in_specs = (
        P(("sp", "tp"), None),
        P("sp", "tp"),
        P("sp", "tp"),
        P("sp", "tp"),
        P(),
        P(),
        P("tp", None),
        P(),
        P(),
        P(("sp", "tp"), None),
        P(("sp", "tp")),
        P(("sp", "tp"), None),
        P("sp", None, "tp"),
        P("sp", None, "tp"),
        P("sp", "tp", None),
    )
    out_specs = P(("sp", "tp"), None)
    return jax.shard_map(
        per_device, mesh=mesh, in_specs=in_specs, out_specs=out_specs, check_vma=False
    )
```

```python
import functools

import jax
import jax.numpy as jnp
from jax import lax
from jax.experimental import pallas as pl
from jax.experimental.pallas import tpu as pltpu
from jax.sharding import PartitionSpec as P

GRID_W = 64


deep_alpha = 2.0**0.5
rope_theta = 10000.0


def apply_rotary_heads(block, gain, grid_positions):
    values32 = block.astype(jnp.float32)
    normed = values32 * lax.rsqrt(jnp.mean(values32 * values32, -1, keepdims=True) + 1e-06) * gain
    half = normed.shape[-1] // 2
    inv_freq = rope_theta ** (-jnp.arange(0, half, 2, dtype=jnp.float32) / half)
    grid_row = (grid_positions // GRID_W).astype(jnp.float32)
    grid_col = (grid_positions % GRID_W).astype(jnp.float32)
    angle = jnp.concatenate([grid_row[:, None] * inv_freq, grid_col[:, None] * inv_freq], -1)[
        :, None, :
    ]
    cosine = jnp.cos(angle)
    sine = jnp.sin(angle)
    first = normed[..., :half]
    second = normed[..., half:]
    turned = jnp.concatenate([first * cosine - second * sine, first * sine + second * cosine], -1)
    return turned.astype(jnp.bfloat16)


def layer_norm_gain(summed, gain):
    centre = summed - jnp.mean(summed, -1, keepdims=True)
    spread = jnp.mean(centre * centre, -1, keepdims=True)
    return centre * lax.rsqrt(spread + 1e-06) * gain


MESH = pl.DeviceIdType.MESH


def flip_bits(a, b, size):
    out = 0
    bit = 1
    while bit < size:
        out = out + ((a // bit + b // bit) % 2) * bit
        bit *= 2
    return out


def at_sp(index):
    return {"sp": index}


def at_tp(index):
    return {"tp": index}


def tp_partners(n_tp):
    t = lax.axis_index("tp")
    t1 = t + 1 - 2 * (t % 2)
    t2 = (t + n_tp // 2) % n_tp
    t3 = (t1 + n_tp // 2) % n_tp
    return t, t1, t2, t3


def attn_kernel(n_sp, heads, kv_heads, width, exponent_scale, q_ref, kv_ref, w_hbm, o_ref, slots, m_s, l_s, acc, attn, w, local, send, recv):
    me = lax.axis_index("sp")
    pair = me + 1 - 2 * (me % 2)
    group = heads // kv_heads
    load = pltpu.make_async_copy(w_hbm, w, local.at[0])
    load.start()

    barrier = pltpu.get_barrier_semaphore()
    pl.semaphore_signal(barrier, inc=1, device_id=at_sp(pair), device_id_type=MESH)

    def greet(j, _):
        pl.semaphore_signal(
            barrier, inc=1, device_id=at_sp(flip_bits(me, 2 * j, n_sp)), device_id_type=MESH
        )
        return 0

    lax.fori_loop(1, n_sp // 2, greet, 0)
    pl.semaphore_wait(barrier, n_sp // 2)

    def copy(src, slot, target):
        return pltpu.make_async_remote_copy(
            src_ref=src,
            dst_ref=slots.at[slot],
            send_sem=send.at[slot],
            recv_sem=recv.at[slot],
            device_id=at_sp(target),
            device_id_type=MESH,
        )

    copy(kv_ref, 1, pair).start()

    def spread(j, _):
        copy(kv_ref, 2 * j, flip_bits(me, 2 * j, n_sp)).start()
        return 0

    lax.fori_loop(1, n_sp // 2, spread, 0)

    m_s[...] = jnp.full(m_s.shape, -1e30, jnp.float32)
    l_s[...] = jnp.zeros(l_s.shape, jnp.float32)
    acc[...] = jnp.zeros(acc.shape, jnp.float32)

    def process(block):
        for h in range(heads):
            g = h // group
            q = q_ref[:, h * width : (h + 1) * width]
            k = block[:, g * width : (g + 1) * width]
            v = block[:, (kv_heads + g) * width : (kv_heads + g + 1) * width]
            s = lax.dot_general(q, k, (((1,), (1,)), ((), ())), preferred_element_type=jnp.float32)
            m_prev = m_s[h]
            m_new = jnp.maximum(m_prev, jnp.max(s, -1, keepdims=True))
            m_s[h] = m_new
            alpha = jnp.exp2((m_prev - m_new) * exponent_scale)
            p = jnp.exp2((s - m_new[:, :1]) * exponent_scale)
            l_s[h] = l_s[h] * alpha + jnp.sum(p, -1, keepdims=True)
            acc[h] = acc[h] * alpha + jnp.dot(
                p.astype(jnp.bfloat16), v, preferred_element_type=jnp.float32
            )

    process(kv_ref)

    def step(j, _):
        even = 2 * j + 2
        copy(kv_ref, even, pair).wait_recv()
        copy(slots.at[even], even + 1, pair).start()
        copy(kv_ref, even - 1, pair).wait_recv()
        process(slots.at[even - 1])
        process(slots.at[even])
        return 0

    lax.fori_loop(0, n_sp // 2 - 1, step, 0)
    copy(kv_ref, n_sp - 1, pair).wait_recv()
    process(slots.at[n_sp - 1])
    for h in range(heads):
        attn[:, h * width : (h + 1) * width] = (acc[h] / l_s[h]).astype(jnp.bfloat16)
    load.wait()
    columns = w.shape[1]
    strip = 512 if columns % 512 == 0 else columns
    for c in range(0, columns, strip):
        o_ref[:, c : c + strip] = jnp.dot(
            attn[...], w[:, c : c + strip], preferred_element_type=jnp.float32
        ).astype(jnp.bfloat16)

    def drain(slot, _):
        copy(kv_ref, slot, pair).wait_send()
        return 0

    lax.fori_loop(1, n_sp, drain, 0)


def attend(q_rot, kv, out_weight, n_sp, heads, kv_heads, width):
    rows = q_rot.shape[0]
    return pl.pallas_call(
        functools.partial(
            attn_kernel, n_sp, heads, kv_heads, width, width ** (-0.5) * 1.4426950408889634
        ),
        out_shape=jax.ShapeDtypeStruct((rows, out_weight.shape[1]), jnp.bfloat16),
        in_specs=[pl.BlockSpec(memory_space=pltpu.VMEM)] * 2 + [pl.BlockSpec(memory_space=pl.ANY)],
        out_specs=pl.BlockSpec(memory_space=pltpu.VMEM),
        scratch_shapes=[
            pltpu.VMEM((n_sp,) + kv.shape, jnp.bfloat16),
            pltpu.VMEM((heads, rows, 128), jnp.float32),
            pltpu.VMEM((heads, rows, 128), jnp.float32),
            pltpu.VMEM((heads, rows, width), jnp.float32),
            pltpu.VMEM((rows, heads * width), jnp.bfloat16),
            pltpu.VMEM(out_weight.shape, jnp.bfloat16),
            pltpu.SemaphoreType.DMA((1,)),
            pltpu.SemaphoreType.DMA((n_sp,)),
            pltpu.SemaphoreType.DMA((n_sp,)),
        ],
        compiler_params=pltpu.CompilerParams(collective_id=0, has_side_effects=True),
        name="attend",
    )(q_rot, kv, out_weight)


def moe_kernel(
    n_sp,
    n_tp,
    stride,
    out_ref,
    gate_hbm,
    up_hbm,
    down_hbm,
    back,
    w_gate,
    w_up,
    w_down,
    piece,
    rows,
    part,
    from_core,
    from_pair,
    pair_sum,
    total,
    local,
    send,
    recv,
):
    me = lax.axis_index("sp")
    t, t1, t2, t3 = tp_partners(n_tp)
    cap, width = out_ref.shape[1:]
    strip = 1024 if width % 1024 == 0 else width

    loads = [
        pltpu.make_async_copy(src, dst, local.at[i])
        for i, (src, dst) in enumerate(
            ((gate_hbm, w_gate), (up_hbm, w_up), (down_hbm, w_down), (out_ref.at[me], piece.at[me, t]))
        )
    ]
    for load in loads:
        load.start()

    barrier = pltpu.get_barrier_semaphore()
    pl.semaphore_signal(barrier, inc=1, device_id=at_tp(t1), device_id_type=MESH)
    pl.semaphore_signal(barrier, inc=1, device_id=at_tp(t2), device_id_type=MESH)

    def greet(k, _):
        pl.semaphore_signal(
            barrier, inc=1, device_id=at_sp(flip_bits(me, k, n_sp)), device_id_type=MESH
        )
        return 0

    lax.fori_loop(1, n_sp, greet, 0)
    pl.semaphore_wait(barrier, n_sp + 1)

    def order(i):
        return jnp.where(i < 2, i, 2 + (i - 2 + n_sp // 2 - 2) % max(n_sp - 2, 1))

    def copy(src, dst, kind, k, target):
        return pltpu.make_async_remote_copy(
            src_ref=src,
            dst_ref=dst,
            send_sem=send.at[kind, k],
            recv_sem=recv.at[kind, k],
            device_id=target,
            device_id_type=MESH,
        )

    def owner(k):
        return flip_bits(me, k, n_sp)

    def first_copy(k):
        return copy(out_ref.at[owner(k)], piece.at[me, t], 0, k, at_sp(owner(k)))

    def core_forward(k):
        return copy(piece.at[owner(k), t], piece.at[owner(k), t], 1, k, at_tp(t1))

    def pair_forward(k):
        return copy(piece.at[owner(k), t], piece.at[owner(k), t], 2, k, at_tp(t2))

    def relay_copy(k):
        return copy(piece.at[owner(k), t2], piece.at[owner(k), t2], 3, k, at_tp(t1))

    def core_part(k, half):
        lane = t3 if half else t1
        return copy(part.at[k, lane], from_core.at[k, half], 4 + half, k, at_tp(t1))

    def pair_part(k):
        return copy(pair_sum.at[k], from_pair.at[k], 6, k, at_tp(t2))

    def back_copy(k):
        return copy(total.at[k], back.at[me], 7, k, at_sp(owner(k)))

    copy(out_ref.at[me], piece.at[me, t], 2, 0, at_tp(t2)).start()
    copy(out_ref.at[me], piece.at[me, t], 1, 0, at_tp(t1)).start()

    def spread(i, _):
        first_copy(order(i)).start()
        return 0

    lax.fori_loop(1, n_sp, spread, 0)
    rows[...] = jnp.zeros(rows.shape, jnp.float32)
    for load in loads:
        load.wait()

    def stage_forward(k):
        first_copy(k).wait_recv()
        pair_forward(k).start()
        core_forward(k).start()

    def stage_relay(k):
        pair_forward(k).wait_recv()
        relay_copy(k).start()

    def stage_expert(k):
        core_forward(k).wait_recv()
        relay_copy(k).wait_recv()
        source = owner(k)
        for lane in range(n_tp):
            rows[lane * stride : lane * stride + cap, :] = piece[source, lane].astype(jnp.float32)
        gate = jnp.zeros((n_tp * stride, w_gate.shape[1]), jnp.float32)
        up = jnp.zeros((n_tp * stride, w_up.shape[1]), jnp.float32)
        for c in range(0, width, strip):
            x = rows[:, c : c + strip].astype(jnp.bfloat16)
            gate += jnp.dot(x, w_gate[c : c + strip, :], preferred_element_type=jnp.float32)
            up += jnp.dot(x, w_up[c : c + strip, :], preferred_element_type=jnp.float32)
        hidden = (gate / (1.0 + jnp.exp(-gate)) * up).astype(jnp.bfloat16)
        for c in range(0, width, strip):
            y = jnp.dot(hidden, w_down[:, c : c + strip], preferred_element_type=jnp.float32)
            for lane in range(n_tp):
                part[k, lane, :, c : c + strip] = y[lane * stride : lane * stride + cap].astype(
                    jnp.bfloat16
                )
        core_part(k, 1).start()
        core_part(k, 0).start()

    def stage_pair(k):
        core_part(k, 1).wait_recv()
        for c in range(0, width, strip):
            cols = slice(c, c + strip)
            pair_sum[k, :, cols] = (
                part[k, t2, :, cols].astype(jnp.float32)
                + from_core[k, 1, :, cols].astype(jnp.float32)
            ).astype(jnp.bfloat16)
        pair_part(k).start()

    def stage_total(k):
        core_part(k, 0).wait_recv()
        pair_part(k).wait_recv()

        def add(dst, row):
            for c in range(0, width, strip):
                cols = slice(c, c + strip)
                dst[row, :, cols] = (
                    part[k, t, :, cols].astype(jnp.float32)
                    + from_core[k, 0, :, cols].astype(jnp.float32)
                    + from_pair[k, :, cols].astype(jnp.float32)
                ).astype(jnp.bfloat16)

        @pl.when(k == 0)
        def _():
            add(back, me)

        @pl.when(k > 0)
        def _():
            add(total, k)
            back_copy(k).start()

    def tick(i, _):
        @pl.when(jnp.logical_and(i >= 1, i < n_sp))
        def _():
            stage_forward(order(i))

        @pl.when(jnp.logical_and(i >= 1, i < n_sp + 1))
        def _():
            stage_relay(order(i - 1))

        @pl.when(jnp.logical_and(i >= 2, i < n_sp + 2))
        def _():
            stage_pair(order(i - 2))

        @pl.when(i >= 3)
        def _():
            stage_total(order(i - 3))

        @pl.when(jnp.logical_and(i >= 1, i < n_sp + 1))
        def _():
            stage_expert(order(i - 1))

        return 0

    lax.fori_loop(0, n_sp + 3, tick, 0)

    def drain(k, _):
        core_forward(k).wait_send()
        pair_forward(k).wait_send()
        relay_copy(k).wait_send()
        core_part(k, 0).wait_send()
        core_part(k, 1).wait_send()
        pair_part(k).wait_send()
        return 0

    lax.fori_loop(0, n_sp, drain, 0)

    def drain_far(k, _):
        first_copy(k).wait_send()
        back_copy(k).wait()
        return 0

    lax.fori_loop(1, n_sp, drain_far, 0)


def experts(outgoing, gate_proj, up_proj, down_proj, n_sp, n_tp):
    block = outgoing.shape[1:]
    stride = (block[0] + 7) // 8 * 8
    slots = pltpu.VMEM((n_sp,) + block, jnp.bfloat16)
    lanes = pltpu.VMEM((n_sp, n_tp) + block, jnp.bfloat16)
    anywhere = pl.BlockSpec(memory_space=pl.ANY)
    return pl.pallas_call(
        functools.partial(moe_kernel, n_sp, n_tp, stride),
        out_shape=jax.ShapeDtypeStruct(outgoing.shape, jnp.bfloat16),
        in_specs=[pl.BlockSpec(memory_space=pltpu.VMEM), anywhere, anywhere, anywhere],
        out_specs=pl.BlockSpec(memory_space=pltpu.VMEM),
        scratch_shapes=[
            pltpu.VMEM(gate_proj.shape, jnp.bfloat16),
            pltpu.VMEM(up_proj.shape, jnp.bfloat16),
            pltpu.VMEM(down_proj.shape, jnp.bfloat16),
            lanes,
            pltpu.VMEM((n_tp * stride, block[1]), jnp.float32),
            lanes,
            pltpu.VMEM((n_sp, 2) + block, jnp.bfloat16),
            slots,
            slots,
            slots,
            pltpu.SemaphoreType.DMA((4,)),
            pltpu.SemaphoreType.DMA((8, n_sp)),
            pltpu.SemaphoreType.DMA((8, n_sp)),
        ],
        compiler_params=pltpu.CompilerParams(collective_id=1, has_side_effects=True),
        name="experts",
    )(outgoing, gate_proj, up_proj, down_proj)


def reduce_kernel(steps, n_tp, back, part, out, from_core, from_pair, pair_sum, total, send, recv):
    me = lax.axis_index("sp")
    t, t1, t2, t3 = tp_partners(n_tp)

    barrier = pltpu.get_barrier_semaphore()
    pl.semaphore_signal(barrier, inc=1, device_id=at_tp(t1), device_id_type=MESH)
    pl.semaphore_signal(barrier, inc=1, device_id=at_tp(t2), device_id_type=MESH)
    if back:

        def greet(k, _):
            pl.semaphore_signal(
                barrier, inc=1, device_id=at_sp(flip_bits(me, k, steps)), device_id_type=MESH
            )
            return 0

        lax.fori_loop(1, steps, greet, 0)
        pl.semaphore_wait(barrier, steps + 1)
    else:
        pl.semaphore_wait(barrier, 2)

    def order(i):
        return steps - 1 - i

    def block_of(k, lane):
        return flip_bits(me, k, steps) * n_tp + lane if back else lane * steps + k

    def copy(src, dst, kind, k, target):
        return pltpu.make_async_remote_copy(
            src_ref=src,
            dst_ref=dst,
            send_sem=send.at[kind, k],
            recv_sem=recv.at[kind, k],
            device_id=target,
            device_id_type=MESH,
        )

    def core_copy(k, half):
        lane = t3 if half else t1
        return copy(part.at[block_of(k, lane)], from_core.at[k, half], half, k, at_tp(t1))

    def pair_copy(k):
        return copy(pair_sum.at[k], from_pair.at[k], 2, k, at_tp(t2))

    def back_copy(k):
        return copy(total.at[k], out.at[me], 3, k, at_sp(flip_bits(me, k, steps)))

    def first(i, _):
        k = order(i)
        core_copy(k, 1).start()
        core_copy(k, 0).start()
        return 0

    lax.fori_loop(0, steps, first, 0)

    width = part.shape[-1]
    strip = 512 if width % 512 == 0 else width

    def add_pair(k):
        core_copy(k, 1).wait_recv()
        own = block_of(k, t2)
        for c in range(0, width, strip):
            cols = slice(c, c + strip)
            pair_sum[k, :, cols] = (
                part[own, :, cols].astype(jnp.float32)
                + from_core[k, 1, :, cols].astype(jnp.float32)
            ).astype(jnp.bfloat16)
        pair_copy(k).start()

    def add_all(k, dst, row):
        core_copy(k, 0).wait_recv()
        pair_copy(k).wait_recv()
        own = block_of(k, t)
        for c in range(0, width, strip):
            cols = slice(c, c + strip)
            dst[row, :, cols] = (
                part[own, :, cols].astype(jnp.float32)
                + from_core[k, 0, :, cols].astype(jnp.float32)
                + from_pair[k, :, cols].astype(jnp.float32)
            ).astype(jnp.bfloat16)

    def finish(k):
        if back:
            add_all(k, total, k)
            back_copy(k).start()
        else:
            add_all(k, out, k)

    depth = min(2, steps - 1)
    for i in range(depth):
        add_pair(order(i))

    def middle(i, _):
        add_pair(order(i))
        finish(order(i - depth))
        return 0

    lax.fori_loop(depth, steps, middle, 0)
    for i in range(steps - depth, steps - 1):
        finish(order(i))
    if back:
        add_all(0, out, me)
    else:
        finish(0)

    def drain(k, _):
        core_copy(k, 0).wait_send()
        core_copy(k, 1).wait_send()
        pair_copy(k).wait_send()
        return 0

    lax.fori_loop(0, steps, drain, 0)
    if back:

        def drain_back(k, _):
            back_copy(k).wait()
            return 0

        lax.fori_loop(1, steps, drain_back, 0)


def reduce_lanes(part, steps, n_tp, back, collective_id):
    block = part.shape[1:]
    slots = pltpu.VMEM((steps,) + block, jnp.bfloat16)
    return pl.pallas_call(
        functools.partial(reduce_kernel, steps, n_tp, back),
        out_shape=jax.ShapeDtypeStruct((steps,) + block, jnp.bfloat16),
        in_specs=[pl.BlockSpec(memory_space=pltpu.VMEM)],
        out_specs=pl.BlockSpec(memory_space=pltpu.VMEM),
        scratch_shapes=[
            pltpu.VMEM((steps, 2) + block, jnp.bfloat16),
            slots,
            slots,
            slots if back else pltpu.VMEM((1,) + block, jnp.bfloat16),
            pltpu.SemaphoreType.DMA((4, steps)),
            pltpu.SemaphoreType.DMA((4, steps)),
        ],
        compiler_params=pltpu.CompilerParams(collective_id=collective_id, has_side_effects=True),
        name="reduce_back" if back else "reduce_proj",
    )(part)


def per_device(
    resid,
    queries,
    keys,
    values,
    q_gain,
    key_norm_gain,
    out_weight,
    norm1_gain,
    norm2_gain,
    expert_ids,
    group_weight,
    expert_weight,
    gate_proj,
    up_proj,
    down_proj,
):
    local_tokens = queries.shape[0]
    head_size = q_gain.shape[0]
    kv_local = keys.shape[1] // head_size
    query_group = queries.shape[1] // head_size // kv_local
    model_width = resid.shape[1]
    grid_positions = lax.axis_index("sp") * local_tokens + jnp.arange(local_tokens, dtype=jnp.int32)
    q_rot = apply_rotary_heads(
        queries.reshape(local_tokens, kv_local * query_group, head_size), q_gain, grid_positions
    )
    q_rot = q_rot.reshape(local_tokens, kv_local * query_group * head_size)
    rotated_keys = apply_rotary_heads(
        keys.reshape(local_tokens, kv_local, head_size), key_norm_gain, grid_positions
    )
    rotated_keys = rotated_keys.reshape(local_tokens, kv_local * head_size)
    lanes = lax.axis_size("tp")
    sp_count = lax.axis_size("sp")
    own_rows = local_tokens // lanes
    kv = jnp.concatenate([rotated_keys, values], 1)
    proj_part = attend(
        q_rot, kv, out_weight, sp_count, kv_local * query_group, kv_local, head_size
    )
    proj_rows = 16
    proj_steps = own_rows // proj_rows
    proj = reduce_lanes(
        proj_part.reshape(lanes * proj_steps, proj_rows, model_width), proj_steps, lanes, False, 2
    )
    proj = proj.reshape(own_rows, model_width)
    summed = deep_alpha * resid.astype(jnp.float32) + proj.astype(jnp.float32)
    x_one = layer_norm_gain(summed, norm1_gain).astype(jnp.bfloat16)
    top_count = expert_ids.shape[1]
    expert_local = gate_proj.shape[0]
    expert_total = expert_local * sp_count
    capacity = (3 * top_count * own_rows + 2 * expert_total - 1) // (2 * expert_total)
    flat_ids = expert_ids.reshape(-1)
    one_hot = (flat_ids[:, None] == jnp.arange(expert_total, dtype=jnp.int32)[None, :]).astype(
        jnp.int32
    )
    earlier = jnp.cumsum(one_hot, 0) - one_hot
    rank = jnp.sum(earlier * one_hot, 1)
    slot = flat_ids * capacity + rank
    chosen = slot[:, None] == jnp.arange(expert_total * capacity, dtype=jnp.int32)[None, :]
    chosen = chosen.reshape(own_rows, top_count, expert_total * capacity)
    placing = jnp.sum(chosen.astype(jnp.bfloat16), 1)
    outgoing = lax.dot_general(
        placing, x_one, (((0,), (0,)), ((), ())), preferred_element_type=jnp.float32
    ).astype(jnp.bfloat16)
    outgoing = outgoing.reshape(expert_total, capacity, model_width)
    blocks = outgoing.reshape(sp_count, expert_local * capacity, model_width)
    returned = experts(
        blocks,
        gate_proj.reshape(gate_proj.shape[1:]),
        up_proj.reshape(up_proj.shape[1:]),
        down_proj.reshape(down_proj.shape[1:]),
        sp_count,
        lanes,
    )
    returned = returned.reshape(expert_total * capacity, model_width)
    gates = group_weight[:, None] * expert_weight / jnp.sum(expert_weight, -1, keepdims=True)
    combine = jnp.sum(jnp.where(chosen, gates[..., None], 0.0), 1)
    high = lax.reduce_precision(combine, 8, 7)
    both = jnp.concatenate([high, combine - high], 0).astype(jnp.bfloat16)
    picked = jnp.dot(both, returned, preferred_element_type=jnp.float32)
    moe = picked[:own_rows] + picked[own_rows:]
    final = deep_alpha * x_one.astype(jnp.float32) + moe
    return layer_norm_gain(final, norm2_gain).astype(jnp.bfloat16)


def solution(mesh):
    in_specs = (
        P(("sp", "tp"), None),
        P("sp", "tp"),
        P("sp", "tp"),
        P("sp", "tp"),
        P(),
        P(),
        P("tp", None),
        P(),
        P(),
        P(("sp", "tp"), None),
        P(("sp", "tp")),
        P(("sp", "tp"), None),
        P("sp", None, "tp"),
        P("sp", None, "tp"),
        P("sp", "tp", None),
    )
    out_specs = P(("sp", "tp"), None)
    return jax.shard_map(
        per_device, mesh=mesh, in_specs=in_specs, out_specs=out_specs, check_vma=False
    )
```
